32 devices in a mesh: grp: 2 (over x), ep: 16 (over z, y, core), tp: 1.
Axes of the slice: x: 2, y: 2, z: 4, core: 2. Of those that a mesh axis runs over, the one named last changes fastest.
Arguments:
- tokens: bfloat16 [2048, 2048], P(('grp', 'ep')), parts along dimension 0, may hold values from -6 to 6
- norm_gain: float32 [2048], replicated, may hold values from 0.1 to 1.9
- expert_gate: bfloat16 [16, 2048, 512], P('ep', None, 'tp'), may hold values from -0.125 to 0.125
- expert_up: bfloat16 [16, 2048, 512], P('ep', None, 'tp'), may hold values from -0.125 to 0.125
- expert_down: bfloat16 [16, 512, 2048], P('ep', 'tp'), may hold values from -0.25 to 0.25
- shared_gate: bfloat16 [2048, 512], P(None, 'tp'), may hold values from -0.125 to 0.125
- shared_up: bfloat16 [2048, 512], P(None, 'tp'), may hold values from -0.125 to 0.125
- shared_down: bfloat16 [512, 2048], P('tp'), may hold values from -0.25 to 0.25
- routes: int32 [2048, 8], P(('grp', 'ep')), parts along dimension 0, may hold values from 0 to 15, all different within a row; in each aligned block of 64 rows (0 to 63, 64 to 127, ...) at most 64 rows name the same one
- route_weights: float32 [2048, 8], P(('grp', 'ep')), parts along dimension 0, may hold values from 0.05 to 0.6
Outputs:
- mixed: bfloat16 [2048, 2048], P(('grp', 'ep'), 'tp'), parts along dimension 0
The draws below stay inside these ranges and needn't reach their ends.
There are 2 independent parts, one for each index of `grp`. The reference program is written for one: setup_inputs(seed, part) draws one part's arguments, and reference() takes and returns one part's arrays. A program takes and returns all parts, laid end to end along the dimension named above; an argument that names none is the same for every part. Nothing has to cross between parts.
Inputs may be any that keep to these rules, and one draw needn't show every extreme that they name: `routes`: each row names 8 different experts. Within the rows of one index of ep no expert is named more than 64 times, a bound that some block reaches by the rows of some index of ep.
All inputs are finite; a program needn't handle non-finite values.
Results may differ from the reference program's by a relative error of at most 0.0085.
Values may be sent and summed in bfloat16 or wider, within the bound.
A program may use at most 64 MiB of HBM per device.

```python
import math
import jax
import jax.numpy as jnp
import numpy as np
from jax import lax

D = 2048
FF_E = 512
FF_S = 512
TOP_K = 8
TOK_DEV = 64
EXPERTS = 16
TOKENS = 1024
CAP = 64
N_TP = 1


def block_scale(key, dims, cuts, least, top_value):
    loudness, own = 1.0, jax.random.fold_in(key, 6)
    for position, blocks in cuts:
        draws = jnp.exp(jax.random.uniform(jax.random.fold_in(own, position), (blocks,), jnp.float32, least / len(cuts), top_value / len(cuts)))
        loudness = loudness * jnp.repeat(draws, dims[position] // blocks).reshape([-1 if axis == position else 1 for axis in range(len(dims))])
    return loudness


def routed_block(stream_key, own, number, rows, count, top, limit, slope):
    order = jax.random.permutation(stream_key, count)
    heavy_load, usual = shares(count, rows * top, limit, slope, True), shares(count, rows * top, limit, slope, False)
    places = jnp.arange(count)

    def named(tallies, offset_by):
        used = int((tallies > 0).sum())
        fixed = max(1, used // 4)
        shifted = fixed + (places - fixed + offset_by * (used - fixed)) % max(1, count - fixed)
        return jnp.zeros((count,), jnp.int32).at[order[jnp.where(places < fixed, places, shifted)]].set(jnp.asarray(tallies, jnp.int32))

    tallies = jnp.where(number % 4 == 0, named(heavy_load, number // 4), named(usual, number - number // 4 - 1))
    mixed = jax.random.permutation(jax.random.fold_in(own, 3), count)
    donor, sink = mixed[0:count // 2 * 2:2], mixed[1:count // 2 * 2:2]
    room = jnp.minimum(tallies[donor] - 1, limit - tallies[sink]) // 2
    room = jnp.where((donor == order[0]) | (sink == order[0]) | (tallies[sink] == 0), 0, jnp.maximum(room, 0))
    shifted = jax.random.randint(jax.random.fold_in(own, 4), (count // 2,), 0, 1 << 20) % (room + 1)
    tallies = tallies.at[donor].add(-shifted).at[sink].add(shifted)
    labels = jnp.searchsorted(jnp.cumsum(tallies), jnp.arange(rows * top), side="right").astype(jnp.int32)
    listing = labels.reshape(top, rows).T
    listing = listing[jax.random.permutation(jax.random.fold_in(own, 1), rows)]
    offset_by = jax.random.randint(jax.random.fold_in(own, 2), (rows, 1), 0, top)
    return jnp.take_along_axis(listing, (jnp.arange(top)[None, :] + offset_by) % top, axis=1)


def shares(number_of, total, reach, skew, full):
    loads = [(1 << 20) // math.isqrt(standing ** skew) + 1 for standing in range(1, number_of + 1)]
    largest = reach if full else min(reach, max(-(-total // number_of), total * loads[0] // sum(loads)))
    least = 1 if total - largest >= number_of - 1 else 0
    counts, spare = [largest] + [least] * (number_of - 1), total - largest - least * (number_of - 1)
    while spare > 0:
        movable = [i for i in range(1, number_of) if counts[i] < largest] or [i for i in range(1, number_of) if counts[i] < reach]
        mass, left = sum([loads[i] for i in movable]), spare
        for i in movable:
            more = min(reach - counts[i], max(1, left * loads[i] // mass), spare)
            counts[i] = counts[i] + more
            spare = spare - more
    return np.array(counts)


def scatter_about(rng, extent, spread, reach, cuts=(), kind=jnp.bfloat16):
    array = spread * jax.random.normal(rng, extent, jnp.float32)
    if cuts:
        array = array * block_scale(rng, extent, cuts, -0.22, 0.18)
    return jnp.clip(array, -reach, reach).astype(kind)


def setup_inputs(seed: int = 0, part: int = 0) -> dict:
    keys = jax.random.split(jax.random.key(seed), 11)
    part_keys = jax.random.split(jax.random.fold_in(keys[10], part), 11)
    tokens = scatter_about(part_keys[0], (TOKENS, D), 1.0, 6.0, ((0, 16),))
    norm_gain = jnp.clip(1.0 + 0.18 * jax.random.normal(keys[1], (D,), jnp.float32), 0.1, 1.9)
    expert_gate = scatter_about(keys[2], (EXPERTS, D, FF_E), D ** -0.5, 0.125, ((0, 16),))
    expert_up = scatter_about(keys[3], (EXPERTS, D, FF_E), D ** -0.5, 0.125, ((0, 16),))
    expert_down = scatter_about(keys[4], (EXPERTS, FF_E, D), FF_E ** -0.5, 0.25, ((0, 16),))
    shared_gate = scatter_about(keys[5], (D, FF_S), D ** -0.5, 0.125)
    shared_up = scatter_about(keys[6], (D, FF_S), D ** -0.5, 0.125)
    shared_down = scatter_about(keys[7], (FF_S, D), FF_S ** -0.5, 0.25)
    routes_keys = jax.random.split(jax.random.fold_in(part_keys[8], 1), TOKENS // TOK_DEV)
    routes_turns = jax.random.permutation(jax.random.fold_in(part_keys[8], 3), TOKENS // TOK_DEV)
    routes = jax.vmap(lambda own, number: routed_block(jax.random.fold_in(part_keys[8], 2), own, number, TOK_DEV, EXPERTS, TOP_K, CAP, 2))(routes_keys, routes_turns).reshape((TOKENS, TOP_K))
    route_weights = jnp.clip(0.05 + 0.55 * jax.random.uniform(part_keys[9], (TOKENS, TOP_K), jnp.float32) ** block_scale(part_keys[9], (TOKENS, TOP_K), ((0, 16),), -0.2, 0.2), 0.05, 0.6)
    return dict(tokens=tokens, norm_gain=norm_gain, expert_gate=expert_gate, expert_up=expert_up, expert_down=expert_down, shared_gate=shared_gate, shared_up=shared_up, shared_down=shared_down, routes=routes, route_weights=route_weights)


def rms_scaled(values, gain):
    wide = values.astype(jnp.float32)
    scaled = wide * lax.rsqrt(lax.optimization_barrier(jnp.mean(wide * wide, axis=-1, keepdims=True)) + 1e-06)
    return (scaled * gain).astype(jnp.bfloat16)

def split_swiglu(row_block, w_gate, w_up, w_down, blocks):
    gate_proj = jnp.dot(row_block, w_gate, preferred_element_type=jnp.float32)
    up_proj = jnp.dot(row_block, w_up, preferred_element_type=jnp.float32)
    hidden = (jax.nn.silu(gate_proj) * up_proj).astype(jnp.bfloat16)
    step_width = hidden.shape[1] // blocks
    total = jnp.zeros((row_block.shape[0], w_down.shape[1]), jnp.float32)
    for block_index in range(blocks):
        lower = block_index * step_width
        partial_value = jnp.dot(hidden[:, lower:lower + step_width], w_down[lower:lower + step_width], preferred_element_type=jnp.float32)
        partial_value = lax.optimization_barrier(partial_value.astype(jnp.bfloat16))
        total = total + partial_value.astype(jnp.float32)
    return total.astype(jnp.bfloat16)

def reference(tokens, norm_gain, expert_gate, expert_up, expert_down, shared_gate, shared_up, shared_down, routes, route_weights):
    normed = rms_scaled(tokens, norm_gain)
    shared_out = split_swiglu(normed, shared_gate, shared_up, shared_down, N_TP)

    def one_expert(accum, inputs):
        w_gate, w_up, w_down, expert_index = inputs
        output = split_swiglu(normed, w_gate, w_up, w_down, N_TP)
        weight = lax.optimization_barrier(jnp.sum(jnp.where(routes == expert_index, route_weights, jnp.float32(0.0)), axis=1))
        return (accum + weight[:, None] * output.astype(jnp.float32), None)
    start = jnp.zeros(tokens.shape, jnp.float32)
    accum, unused = lax.scan(one_expert, start, (expert_gate, expert_up, expert_down, jnp.arange(EXPERTS, dtype=jnp.int32)))
    return (accum + shared_out.astype(jnp.float32)).astype(jnp.bfloat16)
```

```python
import functools

import jax
import jax.numpy as jnp
from jax import lax
from jax.experimental import pallas as pl
from jax.experimental.pallas import tpu as pltpu
from jax.sharding import PartitionSpec as P


def rms_scaled(values, gain):
    wide = values.astype(jnp.float32)
    scaled = wide * lax.rsqrt(jnp.mean(wide * wide, axis=-1, keepdims=True) + 1e-06)
    return (scaled * gain).astype(jnp.bfloat16)


def swiglu_partial(row_block, w_gate, w_up, w_down):
    gate_proj = jnp.dot(row_block, w_gate, preferred_element_type=jnp.float32)
    up_proj = jnp.dot(row_block, w_up, preferred_element_type=jnp.float32)
    hidden = (jax.nn.silu(gate_proj) * up_proj).astype(jnp.bfloat16)
    partial_value = jnp.dot(hidden, w_down, preferred_element_type=jnp.float32)
    return lax.optimization_barrier(partial_value.astype(jnp.bfloat16)).astype(jnp.float32)


def per_device(
    tokens,
    norm_gain,
    expert_gate,
    expert_up,
    expert_down,
    shared_gate,
    shared_up,
    shared_down,
    routes,
    route_weights,
):
    tok_rows = tokens.shape[0]
    model_width = tokens.shape[1]
    top_count = routes.shape[1]
    experts = lax.axis_size("ep")
    half_width = model_width // lax.axis_size("tp")
    capacity = min(tok_rows, 2 * tok_rows * top_count // experts)
    normed = rms_scaled(tokens, norm_gain)
    shared_part = swiglu_partial(normed, shared_gate, shared_up, shared_down)
    all_normed = lax.all_gather(normed, "ep", axis=0, tiled=True)
    all_routes = lax.all_gather(routes, "ep", axis=0, tiled=True)
    all_weights = lax.all_gather(route_weights, "ep", axis=0, tiled=True)
    own_expert = lax.axis_index("ep")
    hit_table = all_routes == own_expert
    is_mine = jnp.sum(hit_table.astype(jnp.int32), axis=1).reshape(experts, tok_rows)
    weight_mine = jnp.sum(jnp.where(hit_table, all_weights, jnp.float32(0.0)), axis=1).reshape(
        experts, tok_rows
    )
    slot_rank = jnp.cumsum(is_mine, axis=1) - is_mine
    matches = (slot_rank[:, None, :] == jnp.arange(capacity, dtype=jnp.int32)[None, :, None]) & (
        is_mine[:, None, :] == 1
    )
    slot_token = jnp.sum(
        jnp.where(matches, jnp.arange(tok_rows, dtype=jnp.int32)[None, None, :], 0), axis=2
    )
    slot_live = jnp.any(matches, axis=2).reshape(-1)
    slot_weight = jnp.sum(
        jnp.where(matches, weight_mine[:, None, :], jnp.float32(0.0)), axis=2
    ).reshape(-1)
    global_row = (jnp.arange(experts, dtype=jnp.int32)[:, None] * tok_rows + slot_token).reshape(-1)
    taken = jnp.take(all_normed, global_row, axis=0)
    inbound = jnp.where(slot_live[:, None], taken, jnp.zeros_like(taken))
    expert_part = swiglu_partial(inbound, expert_gate[0], expert_up[0], expert_down[0])
    expert_sum, shared_sum = (
        lax.psum_scatter(
            expert_part.astype(jnp.bfloat16), "tp", scatter_dimension=1, tiled=True
        ).astype(jnp.float32),
        lax.psum_scatter(
            shared_part.astype(jnp.bfloat16), "tp", scatter_dimension=1, tiled=True
        ).astype(jnp.float32),
    )
    expert_out = expert_sum.astype(jnp.bfloat16)
    shared_out = shared_sum.astype(jnp.bfloat16)
    weighted_rows = expert_out.astype(jnp.float32) * slot_weight[:, None]
    terms = (
        jnp.zeros((experts * tok_rows, half_width), jnp.float32).at[global_row].add(weighted_rows)
    )
    routed = lax.psum_scatter(terms, "ep", scatter_dimension=0, tiled=True)
    return (routed + shared_out.astype(jnp.float32)).astype(jnp.bfloat16)


RING_SENDS = ((3, 1, None), (4, 0, None), (2, 1, 0), (3, 0, 1), (1, 1, 2), (2, 0, 3), (1, 0, 5))
LAST_IN = (6, 4)


def remote(src, dst, send_sem, recv_sem, target):
    return pltpu.make_async_remote_copy(
        src_ref=src,
        dst_ref=dst,
        send_sem=send_sem,
        recv_sem=recv_sem,
        device_id={"ep": target},
        device_id_type=pl.DeviceIdType.MESH,
    )


def moe_kernel(
    chips,
    tok_ref,
    gain_ref,
    routes_ref,
    rweights_ref,
    eg_hbm,
    eu_hbm,
    ed_hbm,
    sg_hbm,
    su_hbm,
    sd_hbm,
    out_ref,
    rows,
    part,
    mate,
    hid,
    eg,
    eu,
    ed,
    sg,
    su,
    sd,
    sbuf,
    rbuf,
    shared,
    w_sem,
    own_sem,
    ag_send,
    ag_recv,
    dd_send,
    dd_recv,
    y_send,
    y_recv,
    rs_send,
    rs_recv,
):
    width = tok_ref.shape[1]
    quarter = tok_ref.shape[0] // 2
    block = 4 * quarter
    experts = 2 * chips
    depth = chips // 2
    me = lax.axis_index("ep")
    core = me % 2
    side = (me // 2) % 2
    along = me // 4
    spot = along + side * (chips - 1 - 2 * along)

    def device_at(ring_spot):
        s = lax.rem(ring_spot + chips, chips)
        turn = s // depth
        return (s + turn * (chips - 1 - 2 * s)) * 4 + turn * 2 + core

    partner = me + 1 - 2 * core
    ahead = (device_at(spot + 1), device_at(spot - 1))

    barrier = pltpu.get_barrier_semaphore()
    for peer in (ahead[0], ahead[1], partner):
        pl.semaphore_signal(
            barrier, inc=1, device_id={"ep": peer}, device_id_type=pl.DeviceIdType.MESH
        )
    loads = [
        pltpu.make_async_copy(hbm, vmem, w_sem.at[i])
        for i, (hbm, vmem) in enumerate(
            (
                (eg_hbm.at[0], eg),
                (eu_hbm.at[0], eu),
                (ed_hbm.at[0], ed),
                (sg_hbm, sg),
                (su_hbm, su),
                (sd_hbm, sd),
            )
        )
    ]
    for load in loads:
        load.start()

    wide = tok_ref[...].astype(jnp.float32)
    scaled = wide * lax.rsqrt(jnp.mean(wide * wide, axis=-1, keepdims=True) + 1e-06)
    normed = (scaled * gain_ref[...]).astype(jnp.bfloat16)
    rows[0, core, :, :, :width] = normed.reshape(2, quarter, width)
    lane = lax.broadcasted_iota(jnp.int32, (2 * quarter, 128), 1)
    table = jnp.zeros((2 * quarter, 128), jnp.float32)
    for k in range(routes_ref.shape[1]):
        table = table + jnp.where(
            lax.rem(lane, experts) == routes_ref[:, k : k + 1], rweights_ref[:, k : k + 1], 0.0
        )
    coarse = table.astype(jnp.bfloat16).astype(jnp.float32)
    table = jnp.where(lane < experts, coarse, jnp.where(lane < 2 * experts, table - coarse, 0.0))
    rows[0, core, :, :, width:] = table.astype(jnp.bfloat16).reshape(2, quarter, 128)
    pl.semaphore_wait(barrier, 3)

    def spot_of(way, k):
        hops = 1 + k // 2
        half = k % 2 if way == 0 else 1 - k % 2
        slot = 2 * hops - 1 if way == 0 else jnp.minimum(2 * hops, chips - 1)
        return rows.at[slot, core, half]

    def gather_copy(way, k, first=False):
        half = k % 2 if way == 0 else 1 - k % 2
        source = rows.at[0, core, half] if first else spot_of(way, k - 2)
        return remote(
            source, spot_of(way, k), ag_send.at[way, k], ag_recv.at[way, k], ahead[way]
        )

    def arrival(way, k):
        ref = spot_of(way, k)
        return remote(ref, ref, ag_send.at[way, k], ag_recv.at[way, k], ahead[way])

    def across_copy(way, k):
        ref = spot_of(way, k)
        return remote(ref, ref, dd_send.at[way, k], dd_recv.at[way, k], partner)

    def mate_copy(slot):
        return remote(
            part.at[slot, 1 - core], mate.at[slot], y_send.at[slot], y_recv.at[slot], partner
        )

    for k in (0, 1):
        for way in (0, 1):
            gather_copy(way, k, True).start()
    own_copy = remote(rows.at[0, core], rows.at[0, core], own_sem.at[0], own_sem.at[1], partner)
    own_copy.start()

    step = 256

    def hidden_of(x, gate, up, count):
        for lower in range(0, gate.shape[1], step):
            g = jnp.dot(x, gate[:, lower : lower + step], preferred_element_type=jnp.float32)
            u = jnp.dot(x, up[:, lower : lower + step], preferred_element_type=jnp.float32)
            hid[:count, lower : lower + step] = (jax.nn.silu(g) * u).astype(jnp.bfloat16)

    def expert_block(slot):
        x = rows[slot, :, :, :, :width].reshape(block, width)
        extra = rows[slot, :, :, :, width:].reshape(block, 128).astype(jnp.float32)
        where = lax.broadcasted_iota(jnp.int32, (block, 128), 1)
        weight = jnp.sum(
            jnp.where((where == me) | (where == me + experts), extra, 0.0), axis=1, keepdims=True
        )
        hidden_of(x, eg, eu, block)
        for lower in range(0, width, step):
            o = jnp.dot(
                hid[...], ed[:, lower : lower + step], preferred_element_type=jnp.float32
            )
            part[slot, :, :, :, lower : lower + step] = (
                (o * weight).astype(jnp.bfloat16).reshape(2, 2, quarter, step)
            )
        mate_copy(slot).start()

    for load in loads[:3]:
        load.wait()

    last = chips - 2

    def gather_step(u, carry):
        for way in (0, 1):
            arrival(way, u).wait_recv()

            @pl.when(u + 2 <= last)
            def _():
                gather_copy(way, u + 2).start()

            across_copy(way, u).start()

        @pl.when(u == 0)
        def _():
            own_copy.wait_recv()

        first = 2 * ((u + 1) // 2 - 1)

        @pl.when((u > 0) & (u % 2 == 1))
        def _():
            across_copy(0, first).wait_recv()
            across_copy(0, first + 1).wait_recv()

        @pl.when((u > 0) & (u % 2 == 0))
        def _():
            across_copy(1, first).wait_recv()
            across_copy(1, first + 1).wait_recv()

        expert_block(u)
        return carry

    lax.fori_loop(0, chips - 1, gather_step, 0)

    mate_seen = set()

    def ring_copy(way, k):
        return remote(
            sbuf.at[way, k], rbuf.at[way, k], rs_send.at[way, k], rs_recv.at[way, k], ahead[way]
        )

    def ring_send(way, k):
        hops, kind, inbound = RING_SENDS[k]
        slot = min(2 * hops, chips - 1) if way == 0 else 2 * hops - 1
        half = kind if way == 0 else 1 - kind
        if slot not in mate_seen:
            mate_copy(slot).wait_recv()
            mate_seen.add(slot)
        total = part[slot, core, half].astype(jnp.float32) + mate[slot, half].astype(jnp.float32)
        if inbound is not None:
            ring_copy(way, inbound).wait_recv()
            total = total + rbuf[way, inbound].astype(jnp.float32)
        sbuf[way, k] = total.astype(jnp.bfloat16)
        ring_copy(way, k).start()

    ring_send(1, 0)
    for way in (0, 1):
        across_copy(way, last).wait_recv()
    expert_block(chips - 1)
    ring_send(0, 0)
    for way in (0, 1):
        ring_send(way, 1)

    for load in loads[3:]:
        load.wait()
    hidden_of(rows[0, core, :, :, :width].reshape(2 * quarter, width), sg, su, 2 * quarter)
    mate_copy(0).wait_recv()
    for lower in range(0, width, step):
        o = jnp.dot(
            hid[: 2 * quarter, :], sd[:, lower : lower + step], preferred_element_type=jnp.float32
        )
        cut = slice(lower, lower + step)
        shared[:, :, cut] = (
            o.astype(jnp.bfloat16).astype(jnp.float32).reshape(2, quarter, step)
            + part[0, core, :, :, cut].astype(jnp.float32)
            + mate[0, :, :, cut].astype(jnp.float32)
        )

    for k in range(2, len(RING_SENDS)):
        for way in (0, 1):
            ring_send(way, k)

    for half in (1, 0):
        total = shared[half]
        for way in (0, 1):
            k = LAST_IN[half if way == 0 else 1 - half]
            ring_copy(way, k).wait_recv()
            total = total + rbuf[way, k].astype(jnp.float32)
        out_ref[half * quarter : (half + 1) * quarter, :] = total.astype(jnp.bfloat16)

    own_copy.wait_send()
    for way in (0, 1):
        for k in range(last + 1):
            gather_copy(way, k, k < 2).wait_send()
            across_copy(way, k).wait_send()
            ring_copy(way, k).wait_send()
    for slot in range(chips):
        mate_copy(slot).wait_send()


def ring_per_device(
    tokens,
    norm_gain,
    expert_gate,
    expert_up,
    expert_down,
    shared_gate,
    shared_up,
    shared_down,
    routes,
    route_weights,
):
    experts = lax.axis_size("ep")
    chips = experts // 2
    count, width = tokens.shape
    quarter = count // 2
    hidden = expert_gate.shape[2]
    half = jnp.bfloat16
    messages = chips - 1
    whole = pl.BlockSpec(memory_space=pltpu.VMEM)
    stays = pl.BlockSpec(memory_space=pl.ANY)
    dma = pltpu.SemaphoreType.DMA
    flops = 6 * width * hidden * (experts + 1) * count
    return pl.pallas_call(
        functools.partial(moe_kernel, chips),
        out_shape=jax.ShapeDtypeStruct((count, width), half),
        in_specs=[whole] * 4 + [stays] * 6,
        out_specs=whole,
        scratch_shapes=[
            pltpu.VMEM((chips, 2, 2, quarter, width + 128), half),
            pltpu.VMEM((chips, 2, 2, quarter, width), half),
            pltpu.VMEM((chips, 2, quarter, width), half),
            pltpu.VMEM((2 * count, hidden), half),
            pltpu.VMEM((width, hidden), half),
            pltpu.VMEM((width, hidden), half),
            pltpu.VMEM((hidden, width), half),
            pltpu.VMEM((width, hidden), half),
            pltpu.VMEM((width, hidden), half),
            pltpu.VMEM((hidden, width), half),
            pltpu.VMEM((2, messages, quarter, width), half),
            pltpu.VMEM((2, messages, quarter, width), half),
            pltpu.VMEM((2, quarter, width), jnp.float32),
            dma((6,)),
            dma((2,)),
            dma((2, messages)),
            dma((2, messages)),
            dma((2, messages)),
            dma((2, messages)),
            dma((chips,)),
            dma((chips,)),
            dma((2, messages)),
            dma((2, messages)),
        ],
        compiler_params=pltpu.CompilerParams(
            collective_id=0, has_side_effects=True, vmem_limit_bytes=60 * 2**20
        ),
        cost_estimate=pl.CostEstimate(
            flops=flops, bytes_accessed=12 * width * hidden, transcendentals=0
        ),
    )(
        tokens,
        norm_gain.reshape(1, width),
        routes,
        route_weights,
        expert_gate,
        expert_up,
        expert_down,
        shared_gate,
        shared_up,
        shared_down,
    )


def solution(mesh):
    in_specs = (
        P(("grp", "ep"), None),
        P(),
        P("ep", None, "tp"),
        P("ep", None, "tp"),
        P("ep", "tp", None),
        P(None, "tp"),
        P(None, "tp"),
        P("tp", None),
        P(("grp", "ep"), None),
        P(("grp", "ep"), None),
    )
    out_specs = P(("grp", "ep"), "tp")
    ring = mesh.shape["tp"] == 1 and mesh.shape["ep"] == 16
    return jax.shard_map(
        ring_per_device if ring else per_device,
        mesh=mesh,
        in_specs=in_specs,
        out_specs=out_specs,
        check_vma=False,
    )
```

```python
import functools

import jax
import jax.numpy as jnp
from jax import lax
from jax.experimental import pallas as pl
from jax.experimental.pallas import tpu as pltpu
from jax.sharding import PartitionSpec as P


def rms_scaled(values, gain):
    wide = values.astype(jnp.float32)
    scaled = wide * lax.rsqrt(jnp.mean(wide * wide, axis=-1, keepdims=True) + 1e-06)
    return (scaled * gain).astype(jnp.bfloat16)


def swiglu_partial(row_block, w_gate, w_up, w_down):
    gate_proj = jnp.dot(row_block, w_gate, preferred_element_type=jnp.float32)
    up_proj = jnp.dot(row_block, w_up, preferred_element_type=jnp.float32)
    hidden = (jax.nn.silu(gate_proj) * up_proj).astype(jnp.bfloat16)
    partial_value = jnp.dot(hidden, w_down, preferred_element_type=jnp.float32)
    return lax.optimization_barrier(partial_value.astype(jnp.bfloat16)).astype(jnp.float32)


def per_device(
    tokens,
    norm_gain,
    expert_gate,
    expert_up,
    expert_down,
    shared_gate,
    shared_up,
    shared_down,
    routes,
    route_weights,
):
    tok_rows = tokens.shape[0]
    model_width = tokens.shape[1]
    top_count = routes.shape[1]
    experts = lax.axis_size("ep")
    half_width = model_width // lax.axis_size("tp")
    capacity = min(tok_rows, 2 * tok_rows * top_count // experts)
    normed = rms_scaled(tokens, norm_gain)
    shared_part = swiglu_partial(normed, shared_gate, shared_up, shared_down)
    all_normed = lax.all_gather(normed, "ep", axis=0, tiled=True)
    all_routes = lax.all_gather(routes, "ep", axis=0, tiled=True)
    all_weights = lax.all_gather(route_weights, "ep", axis=0, tiled=True)
    own_expert = lax.axis_index("ep")
    hit_table = all_routes == own_expert
    is_mine = jnp.sum(hit_table.astype(jnp.int32), axis=1).reshape(experts, tok_rows)
    weight_mine = jnp.sum(jnp.where(hit_table, all_weights, jnp.float32(0.0)), axis=1).reshape(
        experts, tok_rows
    )
    slot_rank = jnp.cumsum(is_mine, axis=1) - is_mine
    matches = (slot_rank[:, None, :] == jnp.arange(capacity, dtype=jnp.int32)[None, :, None]) & (
        is_mine[:, None, :] == 1
    )
    slot_token = jnp.sum(
        jnp.where(matches, jnp.arange(tok_rows, dtype=jnp.int32)[None, None, :], 0), axis=2
    )
    slot_live = jnp.any(matches, axis=2).reshape(-1)
    slot_weight = jnp.sum(
        jnp.where(matches, weight_mine[:, None, :], jnp.float32(0.0)), axis=2
    ).reshape(-1)
    global_row = (jnp.arange(experts, dtype=jnp.int32)[:, None] * tok_rows + slot_token).reshape(-1)
    taken = jnp.take(all_normed, global_row, axis=0)
    inbound = jnp.where(slot_live[:, None], taken, jnp.zeros_like(taken))
    expert_part = swiglu_partial(inbound, expert_gate[0], expert_up[0], expert_down[0])
    expert_sum, shared_sum = (
        lax.psum_scatter(
            expert_part.astype(jnp.bfloat16), "tp", scatter_dimension=1, tiled=True
        ).astype(jnp.float32),
        lax.psum_scatter(
            shared_part.astype(jnp.bfloat16), "tp", scatter_dimension=1, tiled=True
        ).astype(jnp.float32),
    )
    expert_out = expert_sum.astype(jnp.bfloat16)
    shared_out = shared_sum.astype(jnp.bfloat16)
    weighted_rows = expert_out.astype(jnp.float32) * slot_weight[:, None]
    terms = (
        jnp.zeros((experts * tok_rows, half_width), jnp.float32).at[global_row].add(weighted_rows)
    )
    routed = lax.psum_scatter(terms, "ep", scatter_dimension=0, tiled=True)
    return (routed + shared_out.astype(jnp.float32)).astype(jnp.bfloat16)


RING_SENDS = (
    (3, 1, 0, None),
    (3, 1, 1, None),
    (4, 0, 0, None),
    (4, 0, 1, None),
    (2, 1, 0, 0),
    (2, 1, 1, 1),
    (3, 0, 0, 2),
    (3, 0, 1, 3),
    (1, 1, 0, 4),
    (2, 0, 0, 6),
    (2, 0, 1, 7),
    (1, 1, 1, 5),
    (1, 0, 0, 9),
    (1, 0, 1, 10),
)
LAST_IN = ((12, 13), (8, 11))


def remote(src, dst, send_sem, recv_sem, target):
    return pltpu.make_async_remote_copy(
        src_ref=src,
        dst_ref=dst,
        send_sem=send_sem,
        recv_sem=recv_sem,
        device_id={"ep": target},
        device_id_type=pl.DeviceIdType.MESH,
    )


def moe_kernel(
    chips,
    tok_ref,
    gain_ref,
    routes_ref,
    rweights_ref,
    eg_hbm,
    eu_hbm,
    ed_hbm,
    sg_hbm,
    su_hbm,
    sd_hbm,
    out_ref,
    rows,
    part,
    mate,
    hid,
    eg,
    eu,
    ed,
    sg,
    su,
    sd,
    sbuf,
    rbuf,
    shared,
    w_sem,
    own_sem,
    ag_send,
    ag_recv,
    dd_send,
    dd_recv,
    y_send,
    y_recv,
    rs_send,
    rs_recv,
):
    width = tok_ref.shape[1]
    quarter = tok_ref.shape[0] // 2
    eighth = quarter // 2
    block = 4 * quarter
    experts = 2 * chips
    depth = chips // 2
    me = lax.axis_index("ep")
    core = me % 2
    side = (me // 2) % 2
    along = me // 4
    spot = along + side * (chips - 1 - 2 * along)

    def device_at(ring_spot):
        s = lax.rem(ring_spot + chips, chips)
        turn = s // depth
        return (s + turn * (chips - 1 - 2 * s)) * 4 + turn * 2 + core

    partner = me + 1 - 2 * core
    ahead = (device_at(spot + 1), device_at(spot - 1))

    barrier = pltpu.get_barrier_semaphore()
    for peer in (ahead[0], ahead[1], partner):
        pl.semaphore_signal(
            barrier, inc=1, device_id={"ep": peer}, device_id_type=pl.DeviceIdType.MESH
        )
    loads = [
        pltpu.make_async_copy(hbm, vmem, w_sem.at[i])
        for i, (hbm, vmem) in enumerate(
            (
                (eg_hbm.at[0], eg),
                (eu_hbm.at[0], eu),
                (ed_hbm.at[0], ed),
                (sg_hbm, sg),
                (su_hbm, su),
                (sd_hbm, sd),
            )
        )
    ]
    for load in loads:
        load.start()

    wide = tok_ref[...].astype(jnp.float32)
    scaled = wide * lax.rsqrt(jnp.mean(wide * wide, axis=-1, keepdims=True) + 1e-06)
    normed = (scaled * gain_ref[...]).astype(jnp.bfloat16)
    rows[0, core, :, :, :width] = normed.reshape(2, quarter, width)
    named = lax.rem(lax.broadcasted_iota(jnp.int32, (128, 2 * quarter), 0), experts)
    table = jnp.zeros((128, 2 * quarter), jnp.float32)
    for k in range(routes_ref.shape[0]):
        table = table + jnp.where(
            named == routes_ref[k : k + 1, :], rweights_ref[k : k + 1, :], 0.0
        )
    table = table.T
    lane = lax.broadcasted_iota(jnp.int32, (2 * quarter, 128), 1)
    coarse = table.astype(jnp.bfloat16).astype(jnp.float32)
    table = jnp.where(lane < experts, coarse, jnp.where(lane < 2 * experts, table - coarse, 0.0))
    rows[0, core, :, :, width:] = table.astype(jnp.bfloat16).reshape(2, quarter, 128)
    pl.semaphore_wait(barrier, 3)

    def spot_of(way, k):
        hops = 1 + k // 2
        half = k % 2 if way == 0 else 1 - k % 2
        slot = 2 * hops - 1 if way == 0 else jnp.minimum(2 * hops, chips - 1)
        return rows.at[slot, core, half]

    def gather_copy(way, k, first=False):
        half = k % 2 if way == 0 else 1 - k % 2
        source = rows.at[0, core, half] if first else spot_of(way, k - 2)
        return remote(
            source, spot_of(way, k), ag_send.at[way, k], ag_recv.at[way, k], ahead[way]
        )

    def arrival(way, k):
        ref = spot_of(way, k)
        return remote(ref, ref, ag_send.at[way, k], ag_recv.at[way, k], ahead[way])

    def across_copy(way, k):
        ref = spot_of(way, k)
        return remote(ref, ref, dd_send.at[way, k], dd_recv.at[way, k], partner)

    def mate_copy(slot):
        return remote(
            part.at[slot, 1 - core], mate.at[slot], y_send.at[slot], y_recv.at[slot], partner
        )

    for k in (0, 1):
        for way in (0, 1):
            gather_copy(way, k, True).start()
    own_copy = remote(rows.at[0, core], rows.at[0, core], own_sem.at[0], own_sem.at[1], partner)
    own_copy.start()

    step = 256

    def hidden_of(x, gate, up, count):
        for lower in range(0, gate.shape[1], step):
            g = jnp.dot(x, gate[:, lower : lower + step], preferred_element_type=jnp.float32)
            u = jnp.dot(x, up[:, lower : lower + step], preferred_element_type=jnp.float32)
            hid[:count, lower : lower + step] = (jax.nn.silu(g) * u).astype(jnp.bfloat16)

    def expert_block(slot):
        x = rows[slot, :, :, :, :width].reshape(block, width)
        extra = rows[slot, :, :, :, width:].reshape(block, 128).astype(jnp.float32)
        where = lax.broadcasted_iota(jnp.int32, (block, 128), 1)
        weight = jnp.sum(
            jnp.where((where == me) | (where == me + experts), extra, 0.0), axis=1, keepdims=True
        )
        hidden_of(x, eg, eu, block)
        for lower in range(0, width, step):
            o = jnp.dot(
                hid[...], ed[:, lower : lower + step], preferred_element_type=jnp.float32
            )
            part[slot, :, :, :, lower : lower + step] = (
                (o * weight).astype(jnp.bfloat16).reshape(2, 4, eighth, step)
            )
        mate_copy(slot).start()

    for load in loads[:3]:
        load.wait()

    last = chips - 2

    def gather_step(u, carry):
        for way in (0, 1):
            arrival(way, u).wait_recv()

            @pl.when(u + 2 <= last)
            def _():
                gather_copy(way, u + 2).start()

            across_copy(way, u).start()

        @pl.when(u == 0)
        def _():
            own_copy.wait_recv()

        first = 2 * ((u + 1) // 2 - 1)

        @pl.when((u > 0) & (u % 2 == 1))
        def _():
            across_copy(0, first).wait_recv()
            across_copy(0, first + 1).wait_recv()

        @pl.when((u > 0) & (u % 2 == 0))
        def _():
            across_copy(1, first).wait_recv()
            across_copy(1, first + 1).wait_recv()

        expert_block(u)
        return carry

    lax.fori_loop(0, last, gather_step, 0)
    for k in (last - 2, last - 1):
        across_copy(1, k).wait_recv()
    expert_block(last)

    mate_seen = set()

    def ring_copy(way, k):
        return remote(
            sbuf.at[way, k], rbuf.at[way, k], rs_send.at[way, k], rs_recv.at[way, k], ahead[way]
        )

    def ring_send(way, k):
        hops, kind, piece, inbound = RING_SENDS[k]
        slot = min(2 * hops, chips - 1) if way == 0 else 2 * hops - 1
        piece = 2 * (kind if way == 0 else 1 - kind) + piece
        if slot not in mate_seen:
            mate_copy(slot).wait_recv()
            mate_seen.add(slot)
        total = part[slot, core, piece].astype(jnp.float32) + mate[slot, piece].astype(jnp.float32)
        if inbound is not None:
            ring_copy(way, inbound).wait_recv()
            total = total + rbuf[way, inbound].astype(jnp.float32)
        sbuf[way, k] = total.astype(jnp.bfloat16)
        ring_copy(way, k).start()

    for way in (1, 0):
        for k in (0, 1):
            ring_send(way, k)
    for way in (0, 1):
        arrival(way, last).wait_recv()
        across_copy(way, last).start()
    for way in (0, 1):
        across_copy(way, last).wait_recv()
    expert_block(chips - 1)
    for way in (0, 1):
        for k in (2, 3):
            ring_send(way, k)

    for load in loads[3:]:
        load.wait()
    hidden_of(rows[0, core, :, :, :width].reshape(2 * quarter, width), sg, su, 2 * quarter)
    mate_copy(0).wait_recv()
    for lower in range(0, width, step):
        o = jnp.dot(
            hid[: 2 * quarter, :], sd[:, lower : lower + step], preferred_element_type=jnp.float32
        )
        cut = slice(lower, lower + step)
        shared[:, :, cut] = (
            o.astype(jnp.bfloat16).astype(jnp.float32).reshape(4, eighth, step)
            + part[0, core, :, :, cut].astype(jnp.float32)
            + mate[0, :, :, cut].astype(jnp.float32)
        )

    for k in range(4, len(RING_SENDS)):
        for way in (0, 1):
            ring_send(way, k)

    for piece in (0, 1, 2, 3):
        total = shared[piece]
        for way in (0, 1):
            half = piece // 2 if way == 0 else 1 - piece // 2
            k = LAST_IN[half][piece % 2]
            ring_copy(way, k).wait_recv()
            total = total + rbuf[way, k].astype(jnp.float32)
        out_ref[piece * eighth : (piece + 1) * eighth, :] = total.astype(jnp.bfloat16)

    own_copy.wait_send()
    for way in (0, 1):
        for k in range(last + 1):
            gather_copy(way, k, k < 2).wait_send()
            across_copy(way, k).wait_send()
        for k in range(len(RING_SENDS)):
            ring_copy(way, k).wait_send()
    for slot in range(chips):
        mate_copy(slot).wait_send()


def ring_per_device(
    tokens,
    norm_gain,
    expert_gate,
    expert_up,
    expert_down,
    shared_gate,
    shared_up,
    shared_down,
    routes,
    route_weights,
):
    experts = lax.axis_size("ep")
    chips = experts // 2
    count, width = tokens.shape
    quarter = count // 2
    hidden = expert_gate.shape[2]
    half = jnp.bfloat16
    messages = chips - 1
    sends = len(RING_SENDS)
    whole = pl.BlockSpec(memory_space=pltpu.VMEM)
    stays = pl.BlockSpec(memory_space=pl.ANY)
    dma = pltpu.SemaphoreType.DMA
    flops = 6 * width * hidden * (experts + 1) * count
    return pl.pallas_call(
        functools.partial(moe_kernel, chips),
        out_shape=jax.ShapeDtypeStruct((count, width), half),
        in_specs=[whole] * 4 + [stays] * 6,
        out_specs=whole,
        scratch_shapes=[
            pltpu.VMEM((chips, 2, 2, quarter, width + 128), half),
            pltpu.VMEM((chips, 2, 4, quarter // 2, width), half),
            pltpu.VMEM((chips, 4, quarter // 2, width), half),
            pltpu.VMEM((2 * count, hidden), half),
            pltpu.VMEM((width, hidden), half),
            pltpu.VMEM((width, hidden), half),
            pltpu.VMEM((hidden, width), half),
            pltpu.VMEM((width, hidden), half),
            pltpu.VMEM((width, hidden), half),
            pltpu.VMEM((hidden, width), half),
            pltpu.VMEM((2, sends, quarter // 2, width), half),
            pltpu.VMEM((2, sends, quarter // 2, width), half),
            pltpu.VMEM((4, quarter // 2, width), jnp.float32),
            dma((6,)),
            dma((2,)),
            dma((2, messages)),
            dma((2, messages)),
            dma((2, messages)),
            dma((2, messages)),
            dma((chips,)),
            dma((chips,)),
            dma((2, sends)),
            dma((2, sends)),
        ],
        compiler_params=pltpu.CompilerParams(
            collective_id=0, has_side_effects=True, vmem_limit_bytes=60 * 2**20
        ),
        cost_estimate=pl.CostEstimate(
            flops=flops, bytes_accessed=12 * width * hidden, transcendentals=0
        ),
    )(
        tokens,
        norm_gain.reshape(1, width),
        routes.T,
        route_weights.T,
        expert_gate,
        expert_up,
        expert_down,
        shared_gate,
        shared_up,
        shared_down,
    )


def solution(mesh):
    in_specs = (
        P(("grp", "ep"), None),
        P(),
        P("ep", None, "tp"),
        P("ep", None, "tp"),
        P("ep", "tp", None),
        P(None, "tp"),
        P(None, "tp"),
        P("tp", None),
        P(("grp", "ep"), None),
        P(("grp", "ep"), None),
    )
    out_specs = P(("grp", "ep"), "tp")
    ring = mesh.shape["tp"] == 1 and mesh.shape["ep"] == 16
    return jax.shard_map(
        ring_per_device if ring else per_device,
        mesh=mesh,
        in_specs=in_specs,
        out_specs=out_specs,
        check_vma=False,
    )
```

```python
import functools

import jax
import jax.numpy as jnp
from jax import lax
from jax.experimental import pallas as pl
from jax.experimental.pallas import tpu as pltpu
from jax.sharding import PartitionSpec as P


def rms_scaled(values, gain):
    wide = values.astype(jnp.float32)
    scaled = wide * lax.rsqrt(jnp.mean(wide * wide, axis=-1, keepdims=True) + 1e-06)
    return (scaled * gain).astype(jnp.bfloat16)


def swiglu_partial(row_block, w_gate, w_up, w_down):
    gate_proj = jnp.dot(row_block, w_gate, preferred_element_type=jnp.float32)
    up_proj = jnp.dot(row_block, w_up, preferred_element_type=jnp.float32)
    hidden = (jax.nn.silu(gate_proj) * up_proj).astype(jnp.bfloat16)
    partial_value = jnp.dot(hidden, w_down, preferred_element_type=jnp.float32)
    return lax.optimization_barrier(partial_value.astype(jnp.bfloat16)).astype(jnp.float32)


def per_device(
    tokens,
    norm_gain,
    expert_gate,
    expert_up,
    expert_down,
    shared_gate,
    shared_up,
    shared_down,
    routes,
    route_weights,
):
    tok_rows = tokens.shape[0]
    model_width = tokens.shape[1]
    top_count = routes.shape[1]
    experts = lax.axis_size("ep")
    half_width = model_width // lax.axis_size("tp")
    capacity = min(tok_rows, 2 * tok_rows * top_count // experts)
    normed = rms_scaled(tokens, norm_gain)
    shared_part = swiglu_partial(normed, shared_gate, shared_up, shared_down)
    all_normed = lax.all_gather(normed, "ep", axis=0, tiled=True)
    all_routes = lax.all_gather(routes, "ep", axis=0, tiled=True)
    all_weights = lax.all_gather(route_weights, "ep", axis=0, tiled=True)
    own_expert = lax.axis_index("ep")
    hit_table = all_routes == own_expert
    is_mine = jnp.sum(hit_table.astype(jnp.int32), axis=1).reshape(experts, tok_rows)
    weight_mine = jnp.sum(jnp.where(hit_table, all_weights, jnp.float32(0.0)), axis=1).reshape(
        experts, tok_rows
    )
    slot_rank = jnp.cumsum(is_mine, axis=1) - is_mine
    matches = (slot_rank[:, None, :] == jnp.arange(capacity, dtype=jnp.int32)[None, :, None]) & (
        is_mine[:, None, :] == 1
    )
    slot_token = jnp.sum(
        jnp.where(matches, jnp.arange(tok_rows, dtype=jnp.int32)[None, None, :], 0), axis=2
    )
    slot_live = jnp.any(matches, axis=2).reshape(-1)
    slot_weight = jnp.sum(
        jnp.where(matches, weight_mine[:, None, :], jnp.float32(0.0)), axis=2
    ).reshape(-1)
    global_row = (jnp.arange(experts, dtype=jnp.int32)[:, None] * tok_rows + slot_token).reshape(-1)
    taken = jnp.take(all_normed, global_row, axis=0)
    inbound = jnp.where(slot_live[:, None], taken, jnp.zeros_like(taken))
    expert_part = swiglu_partial(inbound, expert_gate[0], expert_up[0], expert_down[0])
    expert_sum, shared_sum = (
        lax.psum_scatter(
            expert_part.astype(jnp.bfloat16), "tp", scatter_dimension=1, tiled=True
        ).astype(jnp.float32),
        lax.psum_scatter(
            shared_part.astype(jnp.bfloat16), "tp", scatter_dimension=1, tiled=True
        ).astype(jnp.float32),
    )
    expert_out = expert_sum.astype(jnp.bfloat16)
    shared_out = shared_sum.astype(jnp.bfloat16)
    weighted_rows = expert_out.astype(jnp.float32) * slot_weight[:, None]
    terms = (
        jnp.zeros((experts * tok_rows, half_width), jnp.float32).at[global_row].add(weighted_rows)
    )
    routed = lax.psum_scatter(terms, "ep", scatter_dimension=0, tiled=True)
    return (routed + shared_out.astype(jnp.float32)).astype(jnp.bfloat16)


RING_SENDS = (
    (3, 1, 0, None),
    (3, 1, 1, None),
    (4, 0, 0, None),
    (4, 0, 1, None),
    (2, 1, 0, 0),
    (2, 1, 1, 1),
    (3, 0, 0, 2),
    (3, 0, 1, 3),
    (1, 1, 0, 4),
    (2, 0, 0, 6),
    (2, 0, 1, 7),
    (1, 1, 1, 5),
    (1, 0, 0, 9),
    (1, 0, 1, 10),
)
LAST_IN = ((12, 13), (8, 11))


def remote(src, dst, send_sem, recv_sem, target):
    return pltpu.make_async_remote_copy(
        src_ref=src,
        dst_ref=dst,
        send_sem=send_sem,
        recv_sem=recv_sem,
        device_id={"ep": target},
        device_id_type=pl.DeviceIdType.MESH,
    )


def moe_kernel(
    chips,
    tok_ref,
    gain_ref,
    routes_ref,
    rweights_ref,
    eg_hbm,
    eu_hbm,
    ed_hbm,
    sg_hbm,
    su_hbm,
    sd_hbm,
    out_ref,
    rows,
    tables,
    part,
    mate,
    hid,
    eg,
    eu,
    ed,
    sg,
    su,
    sd,
    sbuf,
    rbuf,
    shared,
    w_sem,
    own_sem,
    ag_send,
    ag_recv,
    dd_send,
    dd_recv,
    tg_send,
    tg_recv,
    td_send,
    td_recv,
    y_send,
    y_recv,
    rs_send,
    rs_recv,
):
    width = tok_ref.shape[1]
    quarter = tok_ref.shape[0] // 2
    eighth = quarter // 2
    block = 4 * quarter
    experts = 2 * chips
    depth = chips // 2
    me = lax.axis_index("ep")
    core = me % 2
    side = (me // 2) % 2
    along = me // 4
    spot = along + side * (chips - 1 - 2 * along)

    def device_at(ring_spot):
        s = lax.rem(ring_spot + chips, chips)
        turn = s // depth
        return (s + turn * (chips - 1 - 2 * s)) * 4 + turn * 2 + core

    partner = me + 1 - 2 * core
    ahead = (device_at(spot + 1), device_at(spot - 1))

    barrier = pltpu.get_barrier_semaphore()
    for peer in (ahead[0], ahead[1], partner):
        pl.semaphore_signal(
            barrier, inc=1, device_id={"ep": peer}, device_id_type=pl.DeviceIdType.MESH
        )
    loads = [
        pltpu.make_async_copy(hbm, vmem, w_sem.at[i])
        for i, (hbm, vmem) in enumerate(
            (
                (eg_hbm.at[0], eg),
                (eu_hbm.at[0], eu),
                (ed_hbm.at[0], ed),
                (sg_hbm, sg),
                (su_hbm, su),
                (sd_hbm, sd),
            )
        )
    ]
    for load in loads:
        load.start()

    wide = tok_ref[...].astype(jnp.float32)
    scaled = wide * lax.rsqrt(jnp.mean(wide * wide, axis=-1, keepdims=True) + 1e-06)
    normed = (scaled * gain_ref[...]).astype(jnp.bfloat16)
    rows[0, core] = normed.reshape(2, quarter, width)
    tally = 2 * quarter
    named = lax.broadcasted_iota(jnp.int32, (experts, 2 * tally), 0)
    twice = jnp.concatenate([routes_ref[...], routes_ref[...]], axis=1)
    worth = jnp.concatenate([rweights_ref[...], rweights_ref[...]], axis=1)
    table = jnp.zeros((experts, 2 * tally), jnp.float32)
    for k in range(routes_ref.shape[0]):
        table = table + jnp.where(named == twice[k : k + 1, :], worth[k : k + 1, :], 0.0)
    coarse = table.astype(jnp.bfloat16).astype(jnp.float32)
    lane = lax.broadcasted_iota(jnp.int32, (experts, 2 * tally), 1)
    tables[0, core] = jnp.where(lane < tally, coarse, table - coarse).astype(jnp.bfloat16)
    pl.semaphore_wait(barrier, 3)

    def spot_of(way, k):
        hops = 1 + k // 2
        half = k % 2 if way == 0 else 1 - k % 2
        slot = 2 * hops - 1 if way == 0 else jnp.minimum(2 * hops, chips - 1)
        return rows.at[slot, core, half]

    def gather_copy(way, k, first=False):
        half = k % 2 if way == 0 else 1 - k % 2
        source = rows.at[0, core, half] if first else spot_of(way, k - 2)
        return remote(
            source, spot_of(way, k), ag_send.at[way, k], ag_recv.at[way, k], ahead[way]
        )

    def arrival(way, k):
        ref = spot_of(way, k)
        return remote(ref, ref, ag_send.at[way, k], ag_recv.at[way, k], ahead[way])

    def across_copy(way, k):
        ref = spot_of(way, k)
        return remote(ref, ref, dd_send.at[way, k], dd_recv.at[way, k], partner)

    def table_at(way, hops):
        return tables.at[2 * hops - 1 if way == 0 else 2 * hops, core]

    def table_copy(way, hops, source):
        return remote(
            source,
            table_at(way, hops),
            tg_send.at[way, hops - 1],
            tg_recv.at[way, hops - 1],
            ahead[way],
        )

    def table_across(way, hops):
        ref = table_at(way, hops)
        return remote(ref, ref, td_send.at[way, hops - 1], td_recv.at[way, hops - 1], partner)

    def mate_copy(slot):
        return remote(
            part.at[slot, 1 - core], mate.at[slot], y_send.at[slot], y_recv.at[slot], partner
        )

    for way in (0, 1):
        table_copy(way, 1, tables.at[0, core]).start()
    for k in (0, 1):
        for way in (0, 1):
            gather_copy(way, k, True).start()
    own_copy = remote(rows.at[0, core], rows.at[0, core], own_sem.at[0], own_sem.at[1], partner)
    own_copy.start()
    own_table = remote(
        tables.at[0, core], tables.at[0, core], own_sem.at[2], own_sem.at[3], partner
    )
    own_table.start()

    step = 256

    def hidden_of(x, gate, up, count):
        for lower in range(0, gate.shape[1], step):
            g = jnp.dot(x, gate[:, lower : lower + step], preferred_element_type=jnp.float32)
            u = jnp.dot(x, up[:, lower : lower + step], preferred_element_type=jnp.float32)
            hid[:count, lower : lower + step] = (jax.nn.silu(g) * u).astype(jnp.bfloat16)

    def expert_block(slot):
        x = rows[slot].reshape(block, width)
        mine = lax.broadcasted_iota(jnp.int32, (2, experts, 2 * tally), 1) == me
        lines = jnp.sum(jnp.where(mine, tables[slot].astype(jnp.float32), 0.0), axis=1)
        lines = lines[:, :tally] + lines[:, tally:]
        line = jnp.concatenate([lines[0:1], lines[1:2]], axis=1)
        weight = jnp.broadcast_to(line, (8, block)).T[:, 0:1]
        hidden_of(x, eg, eu, block)
        for lower in range(0, width, step):
            o = jnp.dot(
                hid[...], ed[:, lower : lower + step], preferred_element_type=jnp.float32
            )
            part[slot, :, :, :, lower : lower + step] = (
                (o * weight).astype(jnp.bfloat16).reshape(2, 4, eighth, step)
            )
        mate_copy(slot).start()

    for load in loads[:3]:
        load.wait()

    last = chips - 2

    def gather_step(u, carry):
        hops = 1 + u // 2

        @pl.when(u % 2 == 0)
        def _():
            for way in (0, 1):
                table_copy(way, hops, table_at(way, hops)).wait_recv()
                table_across(way, hops).start()
            table_copy(0, hops + 1, table_at(0, hops)).start()

            @pl.when(hops < depth - 1)
            def _():
                table_copy(1, hops + 1, table_at(1, hops)).start()

        for way in (0, 1):
            arrival(way, u).wait_recv()

            @pl.when(u + 2 <= last)
            def _():
                gather_copy(way, u + 2).start()

            across_copy(way, u).start()

        @pl.when(u == 0)
        def _():
            own_copy.wait_recv()
            own_table.wait_recv()

        first = 2 * ((u + 1) // 2 - 1)

        @pl.when((u > 0) & (u % 2 == 1))
        def _():
            across_copy(0, first).wait_recv()
            across_copy(0, first + 1).wait_recv()
            table_across(0, 1 + first // 2).wait_recv()

        @pl.when((u > 0) & (u % 2 == 0))
        def _():
            across_copy(1, first).wait_recv()
            across_copy(1, first + 1).wait_recv()
            table_across(1, 1 + first // 2).wait_recv()

        expert_block(u)
        return carry

    lax.fori_loop(0, last, gather_step, 0)
    for k in (last - 2, last - 1):
        across_copy(1, k).wait_recv()
    table_across(1, depth - 1).wait_recv()
    expert_block(last)

    mate_seen = set()

    def ring_copy(way, k):
        return remote(
            sbuf.at[way, k], rbuf.at[way, k], rs_send.at[way, k], rs_recv.at[way, k], ahead[way]
        )

    def ring_send(way, k):
        hops, kind, piece, inbound = RING_SENDS[k]
        slot = min(2 * hops, chips - 1) if way == 0 else 2 * hops - 1
        piece = 2 * (kind if way == 0 else 1 - kind) + piece
        if slot not in mate_seen:
            mate_copy(slot).wait_recv()
            mate_seen.add(slot)
        total = part[slot, core, piece].astype(jnp.float32) + mate[slot, piece].astype(jnp.float32)
        if inbound is not None:
            ring_copy(way, inbound).wait_recv()
            total = total + rbuf[way, inbound].astype(jnp.float32)
        sbuf[way, k] = total.astype(jnp.bfloat16)
        ring_copy(way, k).start()

    for way in (1, 0):
        for k in (0, 1):
            ring_send(way, k)
    table_copy(0, depth, table_at(0, depth)).wait_recv()
    table_across(0, depth).start()
    for way in (0, 1):
        arrival(way, last).wait_recv()
        across_copy(way, last).start()
    for way in (0, 1):
        across_copy(way, last).wait_recv()
    table_across(0, depth).wait_recv()
    expert_block(chips - 1)
    for way in (0, 1):
        for k in (2, 3):
            ring_send(way, k)

    for load in loads[3:]:
        load.wait()
    hidden_of(rows[0, core].reshape(2 * quarter, width), sg, su, 2 * quarter)
    mate_copy(0).wait_recv()
    for lower in range(0, width, step):
        o = jnp.dot(
            hid[: 2 * quarter, :], sd[:, lower : lower + step], preferred_element_type=jnp.float32
        )
        cut = slice(lower, lower + step)
        shared[:, :, cut] = (
            o.astype(jnp.bfloat16).astype(jnp.float32).reshape(4, eighth, step)
            + part[0, core, :, :, cut].astype(jnp.float32)
            + mate[0, :, :, cut].astype(jnp.float32)
        )

    for k in range(4, len(RING_SENDS)):
        for way in (0, 1):
            ring_send(way, k)

    for piece in (0, 1, 2, 3):
        total = shared[piece]
        for way in (0, 1):
            half = piece // 2 if way == 0 else 1 - piece // 2
            k = LAST_IN[half][piece % 2]
            ring_copy(way, k).wait_recv()
            total = total + rbuf[way, k].astype(jnp.float32)
        out_ref[piece * eighth : (piece + 1) * eighth, :] = total.astype(jnp.bfloat16)

    own_copy.wait_send()
    own_table.wait_send()
    for way in (0, 1):
        for hops in range(1, depth + 1 - way):
            table_copy(way, hops, tables.at[0, core]).wait_send()
            table_across(way, hops).wait_send()
    for way in (0, 1):
        for k in range(last + 1):
            gather_copy(way, k, k < 2).wait_send()
            across_copy(way, k).wait_send()
        for k in range(len(RING_SENDS)):
            ring_copy(way, k).wait_send()
    for slot in range(chips):
        mate_copy(slot).wait_send()


def ring_per_device(
    tokens,
    norm_gain,
    expert_gate,
    expert_up,
    expert_down,
    shared_gate,
    shared_up,
    shared_down,
    routes,
    route_weights,
):
    experts = lax.axis_size("ep")
    chips = experts // 2
    count, width = tokens.shape
    quarter = count // 2
    hidden = expert_gate.shape[2]
    half = jnp.bfloat16
    messages = chips - 1
    sends = len(RING_SENDS)
    whole = pl.BlockSpec(memory_space=pltpu.VMEM)
    stays = pl.BlockSpec(memory_space=pl.ANY)
    dma = pltpu.SemaphoreType.DMA
    flops = 6 * width * hidden * (experts + 1) * count
    return pl.pallas_call(
        functools.partial(moe_kernel, chips),
        out_shape=jax.ShapeDtypeStruct((count, width), half),
        in_specs=[whole] * 4 + [stays] * 6,
        out_specs=whole,
        scratch_shapes=[
            pltpu.VMEM((chips, 2, 2, quarter, width), half),
            pltpu.VMEM((chips, 2, experts, 2 * count), half),
            pltpu.VMEM((chips, 2, 4, quarter // 2, width), half),
            pltpu.VMEM((chips, 4, quarter // 2, width), half),
            pltpu.VMEM((2 * count, hidden), half),
            pltpu.VMEM((width, hidden), half),
            pltpu.VMEM((width, hidden), half),
            pltpu.VMEM((hidden, width), half),
            pltpu.VMEM((width, hidden), half),
            pltpu.VMEM((width, hidden), half),
            pltpu.VMEM((hidden, width), half),
            pltpu.VMEM((2, sends, quarter // 2, width), half),
            pltpu.VMEM((2, sends, quarter // 2, width), half),
            pltpu.VMEM((4, quarter // 2, width), jnp.float32),
            dma((6,)),
            dma((4,)),
            dma((2, messages)),
            dma((2, messages)),
            dma((2, messages)),
            dma((2, messages)),
            dma((2, chips // 2)),
            dma((2, chips // 2)),
            dma((2, chips // 2)),
            dma((2, chips // 2)),
            dma((chips,)),
            dma((chips,)),
            dma((2, sends)),
            dma((2, sends)),
        ],
        compiler_params=pltpu.CompilerParams(
            collective_id=0, has_side_effects=True, vmem_limit_bytes=60 * 2**20
        ),
        cost_estimate=pl.CostEstimate(
            flops=flops, bytes_accessed=12 * width * hidden, transcendentals=0
        ),
    )(
        tokens,
        norm_gain.reshape(1, width),
        routes.T,
        route_weights.T,
        expert_gate,
        expert_up,
        expert_down,
        shared_gate,
        shared_up,
        shared_down,
    )


def solution(mesh):
    in_specs = (
        P(("grp", "ep"), None),
        P(),
        P("ep", None, "tp"),
        P("ep", None, "tp"),
        P("ep", "tp", None),
        P(None, "tp"),
        P(None, "tp"),
        P("tp", None),
        P(("grp", "ep"), None),
        P(("grp", "ep"), None),
    )
    out_specs = P(("grp", "ep"), "tp")
    ring = mesh.shape["tp"] == 1 and mesh.shape["ep"] == 16
    return jax.shard_map(
        ring_per_device if ring else per_device,
        mesh=mesh,
        in_specs=in_specs,
        out_specs=out_specs,
        check_vma=False,
    )
```
